32 devices in a mesh: ra: 4 (over z), cb: 2 (over y), dp: 4 (over x, core).
Axes of the slice: x: 2, y: 2, z: 4, core: 2. Of those that a mesh axis runs over, the one named last changes fastest.
Arguments:
- tokens: bfloat16 [1792, 4096], P('dp', 'ra'), may hold values from -70 to 70
- norm_in: bfloat16 [4096], P('ra'), may hold values from 0.099609375 to 1.8984375
- w_up: float32 [4096, 16384], P(None, ('ra', 'cb')), may hold values from -0.09375 to 0.09375
- up_scale: float32 [16384], P(('ra', 'cb')), may hold values from 0.5 to 2
- w_down: float32 [16384, 4096], P('ra', 'cb'), may hold values from -0.0625 to 0.0625
- down_scale: float32 [4096], P('cb'), may hold values from 0.5 to 2
- norm_out: float32 [4096], P('cb'), may hold values from 0.1 to 1.9
Outputs:
- result: bfloat16 [1792, 4096], P('dp', 'cb')
The draws below stay inside these ranges and needn't reach their ends.
All inputs are finite; a program needn't handle non-finite values.
Results may differ from the reference program's by a relative error of at most 0.024.
Values may be sent and summed in bfloat16 or wider, within the bound.
A program may use at most 128 MiB of HBM per device.

```python
import math
import jax
import jax.numpy as jnp
from jax import lax

D = 4096
FF = 16384
TOKENS = 1792
N_RA = 4


def draw_tokens(key, part):
    key_base = jax.random.fold_in(key, 11)
    key_cols = jax.random.fold_in(key, 12)
    key_rows = jax.random.fold_in(key, 13)
    position = jnp.arange(D, dtype=jnp.float32) / D
    col_scale = jnp.exp(jnp.log(10.0) * (position - 0.5)) * jax.random.uniform(key_cols, (D,), jnp.float32, 0.7, 1.4)
    row_scale = jnp.exp(jax.random.uniform(key_rows, (TOKENS, 1), jnp.float32, jnp.log(0.3), jnp.log(3.0)))
    base = jnp.clip(jax.random.normal(key_base, (TOKENS, D), jnp.float32), -5.0, 5.0)
    return (base * col_scale[None, :] * row_scale).astype(jnp.bfloat16)


def with_spikes(array, rng, source, target, shards_of, factor):
    owner, partner = [(jnp.arange(array.shape[dim]) // (array.shape[dim] // shards_of)).reshape([-1 if axis == dim else 1 for axis in range(array.ndim)]) for dim in (source, target)]
    chosen = jax.random.permutation(rng, shards_of)[partner]
    strong = (owner == chosen) | (owner == (partner + shards_of // 2) % shards_of)
    return jnp.where(strong, factor * array, array)


def block_scale(own_key, extent, cuts, smallest, largest):
    loudness = 1.0
    for dim, shards_of in cuts:
        heights = jax.random.uniform(jax.random.fold_in(jax.random.fold_in(own_key, 6), dim), (shards_of,), jnp.float32, smallest / len(cuts), largest / len(cuts))
        loudness = loudness * jnp.repeat(jnp.exp(heights), extent[dim] // shards_of).reshape((-1,) + (1,) * (len(extent) - 1 - dim))
    return loudness


def scatter_about(own_key, extent, width, limit, shards=(), kind=jnp.bfloat16):
    result = jax.random.normal(own_key, extent, jnp.float32) * width
    if len(shards) > 0:
        result = block_scale(own_key, extent, shards, -0.22, 0.18) * result
    return jnp.clip(result, min=-limit, max=limit).astype(kind)


def bell_draw_with(key, shape, spread, limit, cuts, heavy, kind=jnp.bfloat16):
    drawn = spread * jax.random.normal(key, shape, jnp.float32)
    if cuts:
        drawn = drawn * block_scale(key, shape, cuts, -0.22, 0.18)
    return jnp.clip(with_spikes(drawn, jax.random.fold_in(key, 3), *heavy), -limit, limit).astype(kind)


def setup_inputs(seed: int = 0) -> dict:
    keys = jax.random.split(jax.random.key(seed), 8)
    tokens = draw_tokens(jax.random.fold_in(keys[7], 71), 0)
    norm_in = jnp.clip(1.0 + 0.18 * jax.random.normal(keys[1], (D,), jnp.float32), 0.099609375, 1.8984375).astype(jnp.bfloat16)
    w_up = scatter_about(keys[2], (D, FF), D ** -0.5, 0.09375, ((1, 8),), jnp.float32)
    up_scale = jnp.clip(jnp.exp(math.log(2.0) - 1.3862944 * jax.random.uniform(keys[3], (FF,), jnp.float32) ** block_scale(keys[3], (FF,), ((0, 8),), -0.2, 0.2)), 0.5, 2.0)
    w_down = bell_draw_with(keys[4], (FF, D), FF ** -0.5, 0.0625, ((0, 4), (1, 2)), (0, 1, 4, 2.0), jnp.float32)
    down_scale = jnp.clip(jnp.exp(math.log(2.0) - 1.3862944 * jax.random.uniform(keys[5], (D,), jnp.float32) ** block_scale(keys[5], (D,), ((0, 2),), -0.2, 0.2)), 0.5, 2.0)
    norm_out = jnp.clip(1.0 + 0.18 * jax.random.normal(keys[6], (D,), jnp.float32), 0.1, 1.9)
    return dict(tokens=tokens, norm_in=norm_in, w_up=w_up, up_scale=up_scale, w_down=w_down, down_scale=down_scale, norm_out=norm_out)


epsilon = 1e-06
resid_weight = 0.25

def reference(tokens, norm_in, w_up, up_scale, w_down, down_scale, norm_out):
    whole_float = tokens.astype(jnp.float32)
    inv_in = lax.rsqrt(lax.optimization_barrier(jnp.mean(whole_float * whole_float, axis=-1)) + epsilon)
    normed = (whole_float * norm_in.astype(jnp.float32)).astype(jnp.bfloat16)
    pre_act = jnp.dot(normed, w_up.astype(jnp.bfloat16), preferred_element_type=jnp.float32)
    pre_act = pre_act * inv_in[:, None] * up_scale
    hidden = jnp.square(jax.nn.relu(pre_act)).astype(jnp.bfloat16)
    block_rows = FF // N_RA
    weight_blocks = w_down.astype(jnp.bfloat16).reshape(N_RA, block_rows, D)
    hidden_blocks = hidden.reshape(hidden.shape[0], N_RA, block_rows).transpose(1, 0, 2)

    def add_block(total, pair):
        hidden_part, weight_part = pair
        part = jnp.dot(hidden_part, weight_part, preferred_element_type=jnp.float32).astype(jnp.bfloat16)
        part = lax.optimization_barrier(part)
        return (total + part.astype(jnp.float32), None)
    start_total = jnp.zeros((hidden.shape[0], D), jnp.float32)
    down, _ = lax.scan(add_block, start_total, (hidden_blocks, weight_blocks))
    mixed = resid_weight * whole_float + down * down_scale
    inv_out = lax.rsqrt(lax.optimization_barrier(jnp.mean(mixed * mixed, axis=-1)) + epsilon)
    return (mixed * inv_out[:, None] * norm_out).astype(jnp.bfloat16)
```

```python
import functools

import jax
import jax.numpy as jnp
from jax import lax
from jax.experimental import pallas as pl
from jax.experimental.pallas import tpu as pltpu
from jax.sharding import PartitionSpec as P

epsilon = 1e-06
resid_weight = 0.25
MESH = pl.DeviceIdType.MESH
SLOTS = 6
STEP_ROWS = 128
LANES = 128
TILE = 1024
LAG = 2
SHARES = (4, 7, 6, 6, 5)
HALVED = (True, True, True, False, False)


def plain(tokens, norm_in, w_up, up_scale, w_down, down_scale, norm_out):
    whole_rows, whole_gain = (
        lax.all_gather(tokens, "ra", axis=1, tiled=True),
        lax.all_gather(norm_in, "ra", axis=0, tiled=True),
    )
    whole_float = whole_rows.astype(jnp.float32)
    model_width = whole_float.shape[1]
    inv_in = lax.rsqrt(jnp.mean(whole_float * whole_float, axis=-1) + epsilon)
    normed = (whole_float * whole_gain.astype(jnp.float32)).astype(jnp.bfloat16)
    pre_act = jnp.dot(normed, w_up.astype(jnp.bfloat16), preferred_element_type=jnp.float32)
    pre_act = pre_act * inv_in[:, None] * up_scale
    hidden = jnp.square(jax.nn.relu(pre_act)).astype(jnp.bfloat16)
    down_bf = w_down.astype(jnp.bfloat16)
    quarter = down_bf.shape[1]
    partial_value = jnp.dot(
        lax.all_gather(hidden, "cb", axis=1, tiled=True),
        down_bf,
        preferred_element_type=jnp.float32,
    )
    col_block = lax.axis_index("cb")
    x_quarter = lax.dynamic_slice_in_dim(whole_float, col_block * quarter, quarter, 1)
    down = lax.psum(partial_value.astype(jnp.bfloat16), "ra").astype(jnp.float32)
    mixed = resid_weight * x_quarter + down * down_scale
    total_sq = lax.psum(jnp.sum(mixed * mixed, axis=-1), "cb")
    inv_out = lax.rsqrt(total_sq / model_width + epsilon)
    return (mixed * inv_out[:, None] * norm_out).astype(jnp.bfloat16)


def order(n, tiles):
    last = n - 1

    def relays(c, first, stop):
        return [("relay", c, k) for k in range(first, stop)]

    def up(c):
        return [("norm", c)] + [("up", c, j) for j in range(tiles)]

    ops = [("begin", 0), ("gain",), ("begin", 1), ("wu", 0.42), ("relay", 0, 1), ("wu", 0.75)]
    ops += relays(0, 2, last) + [("relay", 1, 1), ("wu", 1.0), ("relay", 0, last), ("begin", 2)]
    ops += relays(1, 2, last) + up(0) + [("relay", 2, 1), ("wd", 0.3), ("relay", 1, last)]
    ops += [("begin", 3), ("wd", 0.55)] + relays(2, 2, last) + [("norm", 1), ("up", 1, 0)]
    ops += [("relay", 2, last)] + [("up", 1, j) for j in range(1, tiles)]
    ops += [("begin", 4), ("relay", 3, 1), ("wd", 0.8)] + relays(3, 2, last) + [("wd", 1.0)]
    ops += [("down", 0)] + up(2) + [("mids", 0), ("relay", 3, last), ("relay", 4, 1)]
    ops += [("down", 1)] + up(3) + relays(4, 2, last) + [("mids", 1), ("relay", 4, last)]
    ops += up(4) + [("down", 2), ("mids", 2), ("down", 3), ("mids", 3), ("down", 4)]
    ops += [("mids", 4)] + [("ends", c) for c in range(5)]
    return ops


def kernel(
    n, plan,
    x_ref, gain_ref, wu_ref, us_ref, wd_ref, ds_ref, no_ref,
    o_ref,
    xa, gains, wu, wd, stage, normed, scale, hid, parts, sums, mixed, lanes, sq, sqr,
    load_sem, own_sem, gs, gr,
    xs, xr, ys, yr, hs, hr, ins, outs, got, qs, qr,
):
    z = lax.axis_index("ra")
    y = lax.axis_index("cb")
    twin = 1 - y
    chunks = len(plan)
    half = xa.shape[3]
    model_width = 2 * n * half
    up_cols = wu.shape[1]
    up_tiles = up_cols // TILE
    steps = wu.shape[0] // STEP_ROWS
    middle = n // 2
    low = z < middle
    inner = jnp.where(low, z + 1, z - 1)
    outer = jnp.where(low, z - 1, z + 1)
    is_mid = (z == middle - 1) | (z == middle)
    has_outer = (z > 0) & (z < n - 1)
    FROM_OUTER, FROM_INNER = 0, 1

    def rows_of(c):
        start, count, _ = plan[c]
        return pl.ds(start, count)

    def load(ref, i, slot):
        return pltpu.make_async_copy(
            ref.at[pl.ds(i * STEP_ROWS, STEP_ROWS)], stage.at[slot], load_sem.at[slot]
        )

    for i in range(SLOTS):
        load(wu_ref, i, i).start()

    def own_piece(c, h):
        return pltpu.make_async_copy(
            x_ref.at[rows_of(c), pl.ds(h * half, half)],
            xa.at[z, h, rows_of(c)],
            own_sem.at[c, h],
        )

    for c in range(chunks):
        for h in range(2):
            own_piece(c, h).start()

    barrier = pltpu.get_barrier_semaphore()
    for j in range(1, n):
        pl.semaphore_signal(
            barrier, inc=1, device_id={"ra": lax.rem(z + j, n)}, device_id_type=MESH
        )
    pl.semaphore_signal(barrier, inc=1, device_id={"cb": twin}, device_id_type=MESH)
    pl.semaphore_wait(barrier, n)

    def remote(src, dst, send, recv, where):
        return pltpu.make_async_remote_copy(
            src_ref=src, dst_ref=dst, send_sem=send, recv_sem=recv,
            device_id=where, device_id_type=MESH,
        )

    def x_copy(c, src, way):
        piece = xa.at[src, y, rows_of(c)] if plan[c][2] else xa.at[src, :, rows_of(c)]
        return remote(piece, piece, xs.at[c, src, way], xr.at[c, src], {"ra": z + 1 - 2 * way})

    def y_copy(c, src):
        piece = xa.at[src, y, rows_of(c)]
        return remote(piece, piece, ys.at[c, src], yr.at[c, src], {"cb": twin})

    def y_arrive(c, src):
        piece = xa.at[src, twin, rows_of(c)]
        return remote(piece, piece, ys.at[c, src], yr.at[c, src], {"cb": twin})

    def start_line(c):
        @pl.when(z + 1 < n)
        def _():
            x_copy(c, z, 0).start()

        @pl.when(z > 0)
        def _():
            x_copy(c, z, 1).start()

    def relay(c, k):
        @pl.when(z - k >= 0)
        def _():
            src = z - k
            x_copy(c, src, 0).wait_recv()

            @pl.when(z + 1 < n)
            def _():
                x_copy(c, src, 0).start()

            if plan[c][2]:
                y_copy(c, src).start()

        @pl.when(z + k < n)
        def _():
            src = z + k
            x_copy(c, src, 1).wait_recv()

            @pl.when(z > 0)
            def _():
                x_copy(c, src, 1).start()

            if plan[c][2]:
                y_copy(c, src).start()

    def gain_copy(where, src):
        return remote(gain_ref, gains.at[src], gs.at[where], gr.at[src], {"ra": where})

    def begin(c):
        for h in range(2):
            own_piece(c, h).wait()
        start_line(c)

    def gain():
        for j in range(1, n):
            gain_copy(lax.rem(z + j, n), z).start()
        gains[z] = gain_ref[...]

    done = {"wu": 0, "wd": 0}

    def convert(name, until):
        ref, target, following = (wu_ref, wu, wd_ref) if name == "wu" else (wd_ref, wd, None)
        first = 0 if following is not None else steps

        def body(i, carry):
            slot = lax.rem(i + first, SLOTS)
            load(ref, i, slot).wait()
            target[pl.ds(pl.multiple_of(i * STEP_ROWS, STEP_ROWS), STEP_ROWS), :] = stage[
                slot
            ].astype(jnp.bfloat16)

            @pl.when(i + SLOTS < steps)
            def _():
                load(ref, i + SLOTS, slot).start()

            if following is not None:
                @pl.when(i + SLOTS >= steps)
                def _():
                    load(following, i + SLOTS - steps, slot).start()

            return carry

        stop = int(steps * until)
        lax.fori_loop(done[name], stop, body, 0)
        done[name] = stop

    def lane_sum(value, total):
        for j in range(value.shape[1] // LANES):
            part = value[:, j * LANES : (j + 1) * LANES]
            total = part if total is None else total + part
        return total

    def hid_copy(c, block, j):
        cols = pl.ds(pl.multiple_of(block * up_cols + j * TILE, TILE), TILE)
        piece = hid.at[rows_of(c), cols]
        return remote(piece, piece, hs.at[c, j], hr.at[c, j], {"cb": twin})

    def norm(c):
        if c == 0:
            for j in range(1, n):
                src = lax.rem(z + j, n)
                gain_copy(src, src).wait_recv()
        if plan[c][2]:
            for j in range(1, n):
                y_arrive(c, lax.rem(z + j, n)).wait_recv()
        rows = plan[c][1]
        total = None
        for s in range(n):
            for h in range(2):
                xf = xa[s, h, rows_of(c)].astype(jnp.float32)
                total = lane_sum(xf * xf, total)
                gain = gains[s][:, h * half : (h + 1) * half]
                lo = (2 * s + h) * half
                normed[:rows, lo : lo + half] = (xf * gain).astype(jnp.bfloat16)
        total = jnp.sum(total, axis=1, keepdims=True)
        inv_in = lax.rsqrt(total / model_width + epsilon)
        scale[:rows] = jnp.broadcast_to(inv_in, (rows, LANES))

    def up(c, j):
        rows = plan[c][1]
        cols = slice(j * TILE, (j + 1) * TILE)
        at = pl.ds(pl.multiple_of(y * up_cols + j * TILE, TILE), TILE)
        pre = jnp.dot(normed[:rows, :], wu[:, cols], preferred_element_type=jnp.float32)
        pre = jnp.maximum(pre * scale[:rows, :1] * us_ref[:, cols], 0.0)
        hid[rows_of(c), at] = (pre * pre).astype(jnp.bfloat16)
        hid_copy(c, y, j).start()

    def inward_copy(c, q, slot):
        return remote(
            parts.at[q, rows_of(c)], sums.at[slot, q, rows_of(c)],
            ins.at[c, q], got.at[c, slot, q], {"ra": inner},
        )

    def send_inward(c, q):
        inward_copy(c, q, jnp.where(is_mid, FROM_INNER, FROM_OUTER)).start()

    def outward_copy(c, q, slot):
        return remote(
            sums.at[slot, q, rows_of(c)], sums.at[FROM_INNER, q, rows_of(c)],
            outs.at[c, q], got.at[c, FROM_INNER, q], {"ra": outer},
        )

    def arrive(c, q, slot):
        piece = sums.at[slot, q, rows_of(c)]
        return remote(piece, piece, ins.at[c, q], got.at[c, slot, q], {"ra": inner})

    def down(c):
        for j in range(up_tiles):
            hid_copy(c, twin, j).wait_recv()
        per = TILE // half

        def body(j, carry):
            cols = pl.ds(pl.multiple_of(j * TILE, TILE), TILE)
            acc = jnp.dot(hid[rows_of(c), :], wd[:, cols], preferred_element_type=jnp.float32)
            for i in range(per):
                q = j * per + i
                parts[q, rows_of(c)] = acc[:, i * half : (i + 1) * half].astype(jnp.bfloat16)

                @pl.when(jnp.logical_not(has_outer))
                def _():
                    send_inward(c, q)

            return carry

        lax.fori_loop(0, n // per, body, 0)

    def inward(c, q):
        arrive(c, q, FROM_OUTER).wait_recv()
        both = parts[q, rows_of(c)].astype(jnp.float32) + sums[
            FROM_OUTER, q, rows_of(c)
        ].astype(jnp.float32)
        parts[q, rows_of(c)] = both.astype(jnp.bfloat16)
        send_inward(c, q)

    def sq_copy(c):
        return remote(sq.at[c], sqr.at[c], qs.at[c], qr.at[c], {"cb": twin})

    def row_blocks(c):
        rows = plan[c][1]
        return [(lo, min(LANES, rows - lo)) for lo in range(0, rows, LANES)]

    def outward(c, q):
        arrive(c, q, FROM_INNER).wait_recv()

        @pl.when(is_mid)
        def _():
            both = parts[q, rows_of(c)].astype(jnp.float32) + sums[
                FROM_INNER, q, rows_of(c)
            ].astype(jnp.float32)
            sums[FROM_OUTER, q, rows_of(c)] = both.astype(jnp.bfloat16)

        slot = jnp.where(is_mid, FROM_OUTER, FROM_INNER)

        @pl.when(has_outer)
        def _():
            outward_copy(c, q, slot).start()

        cols = pl.ds(pl.multiple_of(q * half, half), half)
        at = y * n + q
        resid = xa[lax.div(at, 2), lax.rem(at, 2), rows_of(c)].astype(jnp.float32)
        value = resid_weight * resid + sums[slot, q, rows_of(c)].astype(
            jnp.float32
        ) * ds_ref[:, cols]
        mixed[rows_of(c), cols] = value
        lanes[rows_of(c)] = lane_sum(value * value, lanes[rows_of(c)])

    def send_squares(c):
        rows = plan[c][1]
        total = jnp.sum(lanes[rows_of(c)], axis=1, keepdims=True)
        total = jnp.broadcast_to(total, (rows, LANES))
        for b, (lo, size) in enumerate(row_blocks(c)):
            block = total[lo : lo + size]
            if size < LANES:
                fill = jnp.zeros((LANES - size, LANES), jnp.float32)
                block = jnp.concatenate([block, fill], axis=0)
            sq[c, b] = block.T[:8]
        sq_copy(c).start()

    def clear(c):
        lanes[rows_of(c)] = jnp.zeros((plan[c][1], LANES), jnp.float32)

    def finish(c):
        start, rows, _ = plan[c]
        sq_copy(c).wait_recv()
        for b, (lo, size) in enumerate(row_blocks(c)):
            total = jnp.broadcast_to((sq[c, b] + sqr[c, b])[:1], (LANES, LANES)).T[:size, :1]
            inv_out = lax.rsqrt(total / model_width + epsilon)
            at = pl.ds(start + lo, size)
            o_ref[at, :] = (mixed[at, :] * inv_out * no_ref[...]).astype(jnp.bfloat16)

    def mids(c):
        final = c == chunks - 1

        @pl.when(has_outer)
        def _():
            if c > 0:
                clear(c - 1)
            if final:
                clear(c)

            def body(step, carry):
                inward(c, step)
                if c > 0:
                    outward(c - 1, step)
                if final:
                    @pl.when(step >= LAG)
                    def _():
                        outward(c, step - LAG)

                return carry

            lax.fori_loop(0, n, body, 0)
            if c > 0:
                send_squares(c - 1)
            if c > 1:
                finish(c - 2)
            if final:
                def rest(q, carry):
                    outward(c, q)
                    return carry

                lax.fori_loop(n - LAG, n, rest, 0)
                send_squares(c)
                for done_chunk in range(max(c - 1, 0), chunks):
                    finish(done_chunk)

    def ends(c):
        @pl.when(jnp.logical_not(has_outer))
        def _():
            clear(c)

            def body(q, carry):
                outward(c, q)
                return carry

            lax.fori_loop(0, n, body, 0)
            send_squares(c)
            if c > 0:
                finish(c - 1)
            if c == chunks - 1:
                finish(c)

    table = {
        "begin": begin, "gain": gain, "relay": relay, "up": up, "down": down,
        "norm": norm, "mids": mids, "ends": ends,
        "wu": functools.partial(convert, "wu"), "wd": functools.partial(convert, "wd"),
    }
    for name, *rest in order(n, up_tiles):
        with jax.named_scope("_".join([name] + [str(r) for r in rest])):
            table[name](*rest)

    for j in range(1, n):
        gain_copy(lax.rem(z + j, n), z).wait_send()

    for c in range(chunks):
        for src in range(n):
            @pl.when((src <= z) & (z + 1 < n))
            def _():
                x_copy(c, src, 0).wait_send()

            @pl.when((src >= z) & (z > 0))
            def _():
                x_copy(c, src, 1).wait_send()

            if plan[c][2]:
                @pl.when(z != src)
                def _():
                    y_copy(c, src).wait_send()

        for j in range(up_tiles):
            hid_copy(c, y, j).wait_send()

        for q in range(n):
            inward_copy(c, q, FROM_OUTER).wait_send()

            @pl.when(has_outer)
            def _():
                outward_copy(c, q, FROM_OUTER).wait_send()

        sq_copy(c).wait_send()


def split_rows(total):
    unit, whole = 16, sum(SHARES)
    if total % (unit * whole):
        return None
    plan, start = [], 0
    for share, halved in zip(SHARES, HALVED):
        count = total * share // whole
        plan.append((start, count, halved))
        start += count
    return tuple(plan)


def fused(n, plan, tokens, norm_in, w_up, up_scale, w_down, down_scale, norm_out):
    chunks = len(plan)
    total_rows = tokens.shape[0]
    most = max(count for _, count, _ in plan)
    half = tokens.shape[1] // 2
    wide = w_down.shape[1]
    up_cols = w_up.shape[1]
    blocks = -(-most // LANES)
    bf16, f32 = jnp.bfloat16, jnp.float32
    dma = pltpu.SemaphoreType.DMA
    vmem = pl.BlockSpec(memory_space=pltpu.VMEM)
    far = pl.BlockSpec(memory_space=pl.ANY)
    flops = 2 * tokens.shape[0] * (w_up.size + w_down.size)
    return pl.pallas_call(
        functools.partial(kernel, n, plan),
        out_shape=jax.ShapeDtypeStruct((tokens.shape[0], wide), bf16),
        in_specs=[far, vmem, far, vmem, far, vmem, vmem],
        out_specs=vmem,
        scratch_shapes=[
            pltpu.VMEM((n, 2, total_rows, half), bf16),
            pltpu.VMEM((n, 1, 2 * half), f32),
            pltpu.VMEM(w_up.shape, bf16),
            pltpu.VMEM(w_down.shape, bf16),
            pltpu.VMEM((SLOTS, STEP_ROWS, wide), f32),
            pltpu.VMEM((most, 2 * half * n), bf16),
            pltpu.VMEM((most, LANES), f32),
            pltpu.VMEM((total_rows, 2 * up_cols), bf16),
            pltpu.VMEM((n, total_rows, half), bf16),
            pltpu.VMEM((2, n, total_rows, half), bf16),
            pltpu.VMEM((total_rows, wide), f32),
            pltpu.VMEM((total_rows, LANES), f32),
            pltpu.VMEM((chunks, blocks, 8, LANES), f32),
            pltpu.VMEM((chunks, blocks, 8, LANES), f32),
            dma((SLOTS,)),
            dma((chunks, 2)),
            dma((n,)),
            dma((n,)),
            dma((chunks, n, 2)),
            dma((chunks, n)),
            dma((chunks, n)),
            dma((chunks, n)),
            dma((chunks, up_cols // TILE)),
            dma((chunks, up_cols // TILE)),
            dma((chunks, n)),
            dma((chunks, n)),
            dma((chunks, 2, n)),
            dma((chunks,)),
            dma((chunks,)),
        ],
        compiler_params=pltpu.CompilerParams(
            collective_id=0, has_side_effects=True, vmem_limit_bytes=67043328
        ),
        cost_estimate=pl.CostEstimate(
            flops=flops, bytes_accessed=4 * (w_up.size + w_down.size), transcendentals=0
        ),
    )(
        tokens,
        norm_in.astype(f32)[None, :],
        w_up,
        up_scale[None, :],
        w_down,
        down_scale[None, :],
        norm_out[None, :],
    )


def solution(mesh):
    n, m = mesh.shape["ra"], mesh.shape["cb"]

    def per_device(tokens, norm_in, w_up, up_scale, w_down, down_scale, norm_out):
        args = (tokens, norm_in, w_up, up_scale, w_down, down_scale, norm_out)
        plan = split_rows(tokens.shape[0])
        half = tokens.shape[1] // 2
        fits = (
            m == 2
            and n > 1
            and n % 2 == 0
            and plan is not None
            and tokens.shape[1] % (2 * LANES) == 0
            and TILE % half == 0
            and w_up.shape == w_down.shape
            and w_down.shape[1] == n * half
            and w_up.shape[0] == 2 * n * half
            and w_up.shape[0] % (STEP_ROWS * n) == 0
            and w_up.shape[0] // STEP_ROWS >= SLOTS
            and w_up.shape[1] % TILE == 0
            and w_up.size <= 8 * 1024 * 1024
            and tokens.size * n <= 2 * 1024 * 1024
        )
        return fused(n, plan, *args) if fits else plain(*args)

    placed = (
        P("dp", "ra"),
        P("ra"),
        P(None, ("ra", "cb")),
        P(("ra", "cb")),
        P("ra", "cb"),
        P("cb"),
        P("cb"),
    )
    return jax.shard_map(
        per_device, mesh=mesh, in_specs=placed, out_specs=P("dp", "cb"), check_vma=False
    )
```

```python
import functools

import jax
import jax.numpy as jnp
from jax import lax
from jax.experimental import pallas as pl
from jax.experimental.pallas import tpu as pltpu
from jax.sharding import PartitionSpec as P

epsilon = 1e-06
resid_weight = 0.25
MESH = pl.DeviceIdType.MESH
SLOTS = 6
STEP_ROWS = 128
LANES = 128
TILE = 1024
LAG = 2
SHARES = (4, 7, 7, 6, 4)
HALVED = (True, True, True, False, False)


def plain(tokens, norm_in, w_up, up_scale, w_down, down_scale, norm_out):
    whole_rows, whole_gain = (
        lax.all_gather(tokens, "ra", axis=1, tiled=True),
        lax.all_gather(norm_in, "ra", axis=0, tiled=True),
    )
    whole_float = whole_rows.astype(jnp.float32)
    model_width = whole_float.shape[1]
    inv_in = lax.rsqrt(jnp.mean(whole_float * whole_float, axis=-1) + epsilon)
    normed = (whole_float * whole_gain.astype(jnp.float32)).astype(jnp.bfloat16)
    pre_act = jnp.dot(normed, w_up.astype(jnp.bfloat16), preferred_element_type=jnp.float32)
    pre_act = pre_act * inv_in[:, None] * up_scale
    hidden = jnp.square(jax.nn.relu(pre_act)).astype(jnp.bfloat16)
    down_bf = w_down.astype(jnp.bfloat16)
    quarter = down_bf.shape[1]
    partial_value = jnp.dot(
        lax.all_gather(hidden, "cb", axis=1, tiled=True),
        down_bf,
        preferred_element_type=jnp.float32,
    )
    col_block = lax.axis_index("cb")
    x_quarter = lax.dynamic_slice_in_dim(whole_float, col_block * quarter, quarter, 1)
    down = lax.psum(partial_value.astype(jnp.bfloat16), "ra").astype(jnp.float32)
    mixed = resid_weight * x_quarter + down * down_scale
    total_sq = lax.psum(jnp.sum(mixed * mixed, axis=-1), "cb")
    inv_out = lax.rsqrt(total_sq / model_width + epsilon)
    return (mixed * inv_out[:, None] * norm_out).astype(jnp.bfloat16)


def order(n, tiles):
    last = n - 1

    def relays(c, first, stop):
        return [("relay", c, k) for k in range(first, stop)]

    def up(c):
        return [("norm", c)] + [("up", c, j) for j in range(tiles)]

    ops = [("begin", 0), ("gain",), ("begin", 1), ("wu", 0.42), ("relay", 0, 1), ("wu", 0.75)]
    ops += relays(0, 2, last) + [("relay", 1, 1), ("wu", 1.0), ("relay", 0, last), ("begin", 2)]
    ops += relays(1, 2, last) + up(0) + [("relay", 2, 1), ("wd", 0.25), ("relay", 1, last)]
    ops += [("begin", 3), ("wd", 0.5)] + relays(2, 2, last) + [("wd", 0.75), ("relay", 2, last)]
    ops += [("begin", 4), ("wd", 1.0)] + up(1) + [("relay", 3, 1), ("down", 0)]
    ops += relays(3, 2, last) + [("relay", 4, 1)] + up(2) + [("mids", 0)]
    ops += relays(4, 2, last) + [("relay", 3, last), ("tail", 0), ("down", 1)] + up(3)
    ops += [("relay", 4, last)] + up(4) + [("mids", 1), ("down", 2), ("tail", 1)]
    ops += [("mids", 2), ("down", 3), ("tail", 2), ("mids", 3), ("down", 4), ("tail", 3)]
    ops += [("mids", 4), ("tail", 4)] + [("ends", c) for c in range(5)]
    return ops


def kernel(
    n, plan,
    x_ref, gain_ref, wu_ref, us_ref, wd_ref, ds_ref, no_ref,
    o_ref,
    xa, gains, wu, wd, stage, normed, scale, hid, parts, sums, mixed, lanes, sq, sqr,
    load_sem, own_sem, gs, gr,
    xs, xr, ys, yr, hs, hr, ins, outs, got, qs, qr,
):
    z = lax.axis_index("ra")
    y = lax.axis_index("cb")
    twin = 1 - y
    chunks = len(plan)
    half = xa.shape[3]
    model_width = 2 * n * half
    up_cols = wu.shape[1]
    up_tiles = up_cols // TILE
    steps = wu.shape[0] // STEP_ROWS
    middle = n // 2
    low = z < middle
    inner = jnp.where(low, z + 1, z - 1)
    outer = jnp.where(low, z - 1, z + 1)
    is_mid = (z == middle - 1) | (z == middle)
    has_outer = (z > 0) & (z < n - 1)
    FROM_OUTER, FROM_INNER = 0, 1

    def rows_of(c):
        start, count, _ = plan[c]
        return pl.ds(start, count)

    def load(ref, i, slot):
        return pltpu.make_async_copy(
            ref.at[pl.ds(i * STEP_ROWS, STEP_ROWS)], stage.at[slot], load_sem.at[slot]
        )

    for i in range(SLOTS):
        load(wu_ref, i, i).start()

    def own_piece(c, h):
        return pltpu.make_async_copy(
            x_ref.at[rows_of(c), pl.ds(h * half, half)],
            xa.at[z, h, rows_of(c)],
            own_sem.at[c, h],
        )

    for c in range(chunks):
        for h in range(2):
            own_piece(c, h).start()

    barrier = pltpu.get_barrier_semaphore()
    for j in range(1, n):
        pl.semaphore_signal(
            barrier, inc=1, device_id={"ra": lax.rem(z + j, n)}, device_id_type=MESH
        )
    pl.semaphore_signal(barrier, inc=1, device_id={"cb": twin}, device_id_type=MESH)
    pl.semaphore_wait(barrier, n)

    def remote(src, dst, send, recv, where):
        return pltpu.make_async_remote_copy(
            src_ref=src, dst_ref=dst, send_sem=send, recv_sem=recv,
            device_id=where, device_id_type=MESH,
        )

    def x_copy(c, src, way):
        piece = xa.at[src, y, rows_of(c)] if plan[c][2] else xa.at[src, :, rows_of(c)]
        return remote(piece, piece, xs.at[c, src, way], xr.at[c, src], {"ra": z + 1 - 2 * way})

    def y_copy(c, src):
        piece = xa.at[src, y, rows_of(c)]
        return remote(piece, piece, ys.at[c, src], yr.at[c, src], {"cb": twin})

    def y_arrive(c, src):
        piece = xa.at[src, twin, rows_of(c)]
        return remote(piece, piece, ys.at[c, src], yr.at[c, src], {"cb": twin})

    def start_line(c):
        @pl.when(z + 1 < n)
        def _():
            x_copy(c, z, 0).start()

        @pl.when(z > 0)
        def _():
            x_copy(c, z, 1).start()

    def relay(c, k):
        @pl.when(z - k >= 0)
        def _():
            src = z - k
            x_copy(c, src, 0).wait_recv()

            @pl.when(z + 1 < n)
            def _():
                x_copy(c, src, 0).start()

            if plan[c][2]:
                y_copy(c, src).start()

        @pl.when(z + k < n)
        def _():
            src = z + k
            x_copy(c, src, 1).wait_recv()

            @pl.when(z > 0)
            def _():
                x_copy(c, src, 1).start()

            if plan[c][2]:
                y_copy(c, src).start()

    def gain_copy(where, src):
        return remote(gain_ref, gains.at[src], gs.at[where], gr.at[src], {"ra": where})

    def begin(c):
        for h in range(2):
            own_piece(c, h).wait()
        start_line(c)

    def gain():
        for j in range(1, n):
            gain_copy(lax.rem(z + j, n), z).start()
        gains[z] = gain_ref[...]

    done = {"wu": 0, "wd": 0}

    def convert(name, until):
        ref, target, following = (wu_ref, wu, wd_ref) if name == "wu" else (wd_ref, wd, None)
        first = 0 if following is not None else steps

        def body(i, carry):
            slot = lax.rem(i + first, SLOTS)
            load(ref, i, slot).wait()
            target[pl.ds(pl.multiple_of(i * STEP_ROWS, STEP_ROWS), STEP_ROWS), :] = stage[
                slot
            ].astype(jnp.bfloat16)

            @pl.when(i + SLOTS < steps)
            def _():
                load(ref, i + SLOTS, slot).start()

            if following is not None:
                @pl.when(i + SLOTS >= steps)
                def _():
                    load(following, i + SLOTS - steps, slot).start()

            return carry

        stop = int(steps * until)
        lax.fori_loop(done[name], stop, body, 0)
        done[name] = stop

    def lane_sum(value, total):
        for j in range(value.shape[1] // LANES):
            part = value[:, j * LANES : (j + 1) * LANES]
            total = part if total is None else total + part
        return total

    def hid_copy(c, block, j):
        cols = pl.ds(pl.multiple_of(block * up_cols + j * TILE, TILE), TILE)
        piece = hid.at[rows_of(c), cols]
        return remote(piece, piece, hs.at[c, j], hr.at[c, j], {"cb": twin})

    def norm(c):
        if c == 0:
            for j in range(1, n):
                src = lax.rem(z + j, n)
                gain_copy(src, src).wait_recv()
        if plan[c][2]:
            for j in range(1, n):
                y_arrive(c, lax.rem(z + j, n)).wait_recv()
        rows = plan[c][1]
        total = None
        for s in range(n):
            for h in range(2):
                xf = xa[s, h, rows_of(c)].astype(jnp.float32)
                total = lane_sum(xf * xf, total)
                gain = gains[s].astype(jnp.float32)
                lo = (2 * s + h) * half
                for j in range(half // LANES):
                    at = h * (half // LANES) + j
                    part = xf[:, j * LANES : (j + 1) * LANES] * gain[at : at + 1]
                    normed[:rows, lo + j * LANES : lo + (j + 1) * LANES] = part.astype(
                        jnp.bfloat16
                    )
        total = jnp.sum(total, axis=1, keepdims=True)
        inv_in = lax.rsqrt(total / model_width + epsilon)
        scale[:rows] = jnp.broadcast_to(inv_in, (rows, LANES))

    def up(c, j):
        rows = plan[c][1]
        cols = slice(j * TILE, (j + 1) * TILE)
        at = pl.ds(pl.multiple_of(y * up_cols + j * TILE, TILE), TILE)
        pre = jnp.dot(normed[:rows, :], wu[:, cols], preferred_element_type=jnp.float32)
        pre = jnp.maximum(pre * scale[:rows, :1] * us_ref[:, cols], 0.0)
        hid[rows_of(c), at] = (pre * pre).astype(jnp.bfloat16)
        hid_copy(c, y, j).start()

    def inward_copy(c, q, slot):
        return remote(
            parts.at[q, rows_of(c)], sums.at[slot, q, rows_of(c)],
            ins.at[c, q], got.at[c, slot, q], {"ra": inner},
        )

    def send_inward(c, q):
        inward_copy(c, q, jnp.where(is_mid, FROM_INNER, FROM_OUTER)).start()

    def outward_copy(c, q, slot):
        return remote(
            sums.at[slot, q, rows_of(c)], sums.at[FROM_INNER, q, rows_of(c)],
            outs.at[c, q], got.at[c, FROM_INNER, q], {"ra": outer},
        )

    def arrive(c, q, slot):
        piece = sums.at[slot, q, rows_of(c)]
        return remote(piece, piece, ins.at[c, q], got.at[c, slot, q], {"ra": inner})

    def down(c):
        for j in range(up_tiles):
            hid_copy(c, twin, j).wait_recv()
        per = TILE // half

        def body(j, carry):
            cols = pl.ds(pl.multiple_of(j * TILE, TILE), TILE)
            acc = jnp.dot(hid[rows_of(c), :], wd[:, cols], preferred_element_type=jnp.float32)
            for i in range(per):
                q = j * per + i
                parts[q, rows_of(c)] = acc[:, i * half : (i + 1) * half].astype(jnp.bfloat16)

                @pl.when(jnp.logical_not(has_outer))
                def _():
                    send_inward(c, q)

            return carry

        lax.fori_loop(0, n // per, body, 0)

    def inward(c, q):
        arrive(c, q, FROM_OUTER).wait_recv()
        both = parts[q, rows_of(c)].astype(jnp.float32) + sums[
            FROM_OUTER, q, rows_of(c)
        ].astype(jnp.float32)
        parts[q, rows_of(c)] = both.astype(jnp.bfloat16)
        send_inward(c, q)

    def sq_copy(c):
        return remote(sq.at[c], sqr.at[c], qs.at[c], qr.at[c], {"cb": twin})

    def row_blocks(c):
        rows = plan[c][1]
        return [(lo, min(LANES, rows - lo)) for lo in range(0, rows, LANES)]

    def outward(c, q):
        arrive(c, q, FROM_INNER).wait_recv()

        @pl.when(is_mid)
        def _():
            both = parts[q, rows_of(c)].astype(jnp.float32) + sums[
                FROM_INNER, q, rows_of(c)
            ].astype(jnp.float32)
            sums[FROM_OUTER, q, rows_of(c)] = both.astype(jnp.bfloat16)

        slot = jnp.where(is_mid, FROM_OUTER, FROM_INNER)

        @pl.when(has_outer)
        def _():
            outward_copy(c, q, slot).start()

        cols = pl.ds(pl.multiple_of(q * half, half), half)
        at = y * n + q
        resid = xa[lax.div(at, 2), lax.rem(at, 2), rows_of(c)].astype(jnp.float32)
        value = resid_weight * resid + sums[slot, q, rows_of(c)].astype(
            jnp.float32
        ) * ds_ref[:, cols]
        mixed[rows_of(c), cols] = value
        lanes[rows_of(c)] = lane_sum(value * value, lanes[rows_of(c)])

    def send_squares(c):
        rows = plan[c][1]
        total = jnp.sum(lanes[rows_of(c)], axis=1, keepdims=True)
        total = jnp.broadcast_to(total, (rows, LANES))
        for b, (lo, size) in enumerate(row_blocks(c)):
            block = total[lo : lo + size]
            if size < LANES:
                fill = jnp.zeros((LANES - size, LANES), jnp.float32)
                block = jnp.concatenate([block, fill], axis=0)
            sq[c, b] = block.T[:8]
        sq_copy(c).start()

    def clear(c):
        lanes[rows_of(c)] = jnp.zeros((plan[c][1], LANES), jnp.float32)

    def finish(c):
        start, rows, _ = plan[c]
        sq_copy(c).wait_recv()
        for b, (lo, size) in enumerate(row_blocks(c)):
            total = jnp.broadcast_to((sq[c, b] + sqr[c, b])[:1], (LANES, LANES)).T[:size, :1]
            inv_out = lax.rsqrt(total / model_width + epsilon)
            at = pl.ds(start + lo, size)
            o_ref[at, :] = (mixed[at, :] * inv_out * no_ref[...]).astype(jnp.bfloat16)

    def mids(c):
        @pl.when(has_outer)
        def _():
            clear(c)

            def body(step, carry):
                inward(c, step)

                @pl.when(step >= LAG)
                def _():
                    outward(c, step - LAG)

                return carry

            lax.fori_loop(0, n, body, 0)

    def tail(c):
        @pl.when(has_outer)
        def _():
            def body(q, carry):
                outward(c, q)
                return carry

            lax.fori_loop(n - LAG, n, body, 0)
            send_squares(c)
            if c > 0:
                finish(c - 1)
            if c == chunks - 1:
                finish(c)

    def ends(c):
        @pl.when(jnp.logical_not(has_outer))
        def _():
            clear(c)

            def body(q, carry):
                outward(c, q)
                return carry

            lax.fori_loop(0, n, body, 0)
            send_squares(c)
            if c > 0:
                finish(c - 1)
            if c == chunks - 1:
                finish(c)

    table = {
        "begin": begin, "gain": gain, "relay": relay, "up": up, "down": down,
        "norm": norm, "mids": mids, "tail": tail, "ends": ends,
        "wu": functools.partial(convert, "wu"), "wd": functools.partial(convert, "wd"),
    }
    for name, *rest in order(n, up_tiles):
        with jax.named_scope("_".join([name] + [str(r) for r in rest])):
            table[name](*rest)

    for j in range(1, n):
        gain_copy(lax.rem(z + j, n), z).wait_send()

    for c in range(chunks):
        for src in range(n):
            @pl.when((src <= z) & (z + 1 < n))
            def _():
                x_copy(c, src, 0).wait_send()

            @pl.when((src >= z) & (z > 0))
            def _():
                x_copy(c, src, 1).wait_send()

            if plan[c][2]:
                @pl.when(z != src)
                def _():
                    y_copy(c, src).wait_send()

        for j in range(up_tiles):
            hid_copy(c, y, j).wait_send()

        for q in range(n):
            inward_copy(c, q, FROM_OUTER).wait_send()

            @pl.when(has_outer)
            def _():
                outward_copy(c, q, FROM_OUTER).wait_send()

        sq_copy(c).wait_send()


def split_rows(total):
    unit, whole = 16, sum(SHARES)
    if total % (unit * whole):
        return None
    plan, start = [], 0
    for share, halved in zip(SHARES, HALVED):
        count = total * share // whole
        plan.append((start, count, halved))
        start += count
    return tuple(plan)


def fused(n, plan, tokens, norm_in, w_up, up_scale, w_down, down_scale, norm_out):
    chunks = len(plan)
    total_rows = tokens.shape[0]
    most = max(count for _, count, _ in plan)
    half = tokens.shape[1] // 2
    wide = w_down.shape[1]
    up_cols = w_up.shape[1]
    blocks = -(-most // LANES)
    bf16, f32 = jnp.bfloat16, jnp.float32
    dma = pltpu.SemaphoreType.DMA
    vmem = pl.BlockSpec(memory_space=pltpu.VMEM)
    far = pl.BlockSpec(memory_space=pl.ANY)
    flops = 2 * tokens.shape[0] * (w_up.size + w_down.size)
    return pl.pallas_call(
        functools.partial(kernel, n, plan),
        out_shape=jax.ShapeDtypeStruct((tokens.shape[0], wide), bf16),
        in_specs=[far, vmem, far, vmem, far, vmem, vmem],
        out_specs=vmem,
        scratch_shapes=[
            pltpu.VMEM((n, 2, total_rows, half), bf16),
            pltpu.VMEM((n, 2 * half // LANES, LANES), bf16),
            pltpu.VMEM(w_up.shape, bf16),
            pltpu.VMEM(w_down.shape, bf16),
            pltpu.VMEM((SLOTS, STEP_ROWS, wide), f32),
            pltpu.VMEM((most, 2 * half * n), bf16),
            pltpu.VMEM((most, LANES), f32),
            pltpu.VMEM((total_rows, 2 * up_cols), bf16),
            pltpu.VMEM((n, total_rows, half), bf16),
            pltpu.VMEM((2, n, total_rows, half), bf16),
            pltpu.VMEM((total_rows, wide), f32),
            pltpu.VMEM((total_rows, LANES), f32),
            pltpu.VMEM((chunks, blocks, 8, LANES), f32),
            pltpu.VMEM((chunks, blocks, 8, LANES), f32),
            dma((SLOTS,)),
            dma((chunks, 2)),
            dma((n,)),
            dma((n,)),
            dma((chunks, n, 2)),
            dma((chunks, n)),
            dma((chunks, n)),
            dma((chunks, n)),
            dma((chunks, up_cols // TILE)),
            dma((chunks, up_cols // TILE)),
            dma((chunks, n)),
            dma((chunks, n)),
            dma((chunks, 2, n)),
            dma((chunks,)),
            dma((chunks,)),
        ],
        compiler_params=pltpu.CompilerParams(
            collective_id=0, has_side_effects=True, vmem_limit_bytes=67043328
        ),
        cost_estimate=pl.CostEstimate(
            flops=flops, bytes_accessed=4 * (w_up.size + w_down.size), transcendentals=0
        ),
    )(
        tokens,
        norm_in.reshape(-1, LANES),
        w_up,
        up_scale[None, :],
        w_down,
        down_scale[None, :],
        norm_out[None, :],
    )


def solution(mesh):
    n, m = mesh.shape["ra"], mesh.shape["cb"]

    def per_device(tokens, norm_in, w_up, up_scale, w_down, down_scale, norm_out):
        args = (tokens, norm_in, w_up, up_scale, w_down, down_scale, norm_out)
        plan = split_rows(tokens.shape[0])
        half = tokens.shape[1] // 2
        fits = (
            m == 2
            and n > 1
            and n % 2 == 0
            and plan is not None
            and tokens.shape[1] % (2 * LANES) == 0
            and TILE % half == 0
            and w_up.shape == w_down.shape
            and w_down.shape[1] == n * half
            and w_up.shape[0] == 2 * n * half
            and w_up.shape[0] % (STEP_ROWS * n) == 0
            and w_up.shape[0] // STEP_ROWS >= SLOTS
            and w_up.shape[1] % TILE == 0
            and w_up.size <= 8 * 1024 * 1024
            and tokens.size * n <= 2 * 1024 * 1024
        )
        return fused(n, plan, *args) if fits else plain(*args)

    placed = (
        P("dp", "ra"),
        P("ra"),
        P(None, ("ra", "cb")),
        P(("ra", "cb")),
        P("ra", "cb"),
        P("cb"),
        P("cb"),
    )
    return jax.shard_map(
        per_device, mesh=mesh, in_specs=placed, out_specs=P("dp", "cb"), check_vma=False
    )
```
